32 devices in a mesh: sp: 8 (over z, x), tp: 4 (over y, core).
Axes of the slice: x: 2, y: 2, z: 4, core: 2. Of those that a mesh axis runs over, the one named last changes fastest.
Arguments:
- queries: bfloat16 [8192, 1536], P('sp', 'tp'), may hold values from -200 to 200
- key_heads: bfloat16 [8192, 512], P('sp', 'tp'), may hold values from -6 to 6
- projected_value_heads: bfloat16 [8192, 512], P('sp', 'tp'), may hold values from -5 to 5
- sink_logit_table: float32 [24], P('tp'), may hold values from 0 to 4
- out_weight: bfloat16 [1536, 3072], P('tp'), may hold values from -1.5 to 1.5
- residual: bfloat16 [8192, 3072], P('sp', 'tp'), may hold values from -16 to 16
- norm_gain: bfloat16 [3072], P('tp'), may hold values from 0.099609375 to 1.8984375
- up_weight: bfloat16 [3072, 12288], P('sp', 'tp'), may hold values from -0.109375 to 0.109375
- down_weight: bfloat16 [12288, 3072], P('tp', 'sp'), may hold values from -0.0546875 to 0.0546875
Outputs:
- result: bfloat16 [8192, 3072], P('sp', 'tp')
The draws below stay inside these ranges and needn't reach their ends.
All inputs are finite; a program needn't handle non-finite values.
Results may differ from the reference program's by a relative error of at most 0.015.
Values may be sent and summed in bfloat16 or wider, within the bound.
A program may use at most 128 MiB of HBM per device.

```python
import math
import jax
import jax.numpy as jnp
from jax import lax

D = 3072
FF = 12288
QUERY_HEADS = 24
KEY_VALUE_HEADS = 8
HEAD_SIZE = 64
WINDOW_SPAN = 128
SEQUENCE_TOKENS = 8192
N_TP = 4


def inserted_value(key):
    starting_query = jax.random.truncated_normal(jax.random.fold_in(key, 11), -5.0, 5.0, (SEQUENCE_TOKENS, KEY_VALUE_HEADS, QUERY_HEADS // KEY_VALUE_HEADS, HEAD_SIZE), jnp.float32)
    starting_keys = jax.random.truncated_normal(jax.random.fold_in(key, 12), -5.0, 5.0, (SEQUENCE_TOKENS, KEY_VALUE_HEADS, HEAD_SIZE), jnp.float32)
    query_out = starting_query
    keys_out = starting_keys
    return (query_out, keys_out)


def draw_queries(key, part):
    return inserted_value(key)[0].reshape(SEQUENCE_TOKENS, QUERY_HEADS * HEAD_SIZE).astype(jnp.bfloat16)


def draw_key_heads(key, part):
    return inserted_value(key)[1].reshape(SEQUENCE_TOKENS, KEY_VALUE_HEADS * HEAD_SIZE).astype(jnp.bfloat16)


def draw_residual(key, part):
    column = jnp.arange(D).astype(jnp.float32) / (D - 1)
    base = jax.random.truncated_normal(jax.random.fold_in(key, 22), -5.0, 5.0, (SEQUENCE_TOKENS, D), jnp.float32)
    scale = jnp.exp(math.log(3.0) * column)
    return (base * scale[None, :]).astype(jnp.bfloat16)


def shard_levels(rng, dims, split, low, largest):
    def one(position, shards_of):
        steps = jax.random.uniform(jax.random.fold_in(jax.random.fold_in(rng, 6), position), (shards_of,), jnp.float32, low / len(split), largest / len(split))
        return jnp.repeat(jnp.exp(steps), dims[position] // shards_of).reshape((-1,) + (1,) * (len(dims) - position - 1))

    loudness = one(*split[0])
    for cut in split[1:]:
        loudness = loudness * one(*cut)
    return loudness


def noise(stream_key, shape, width, reach, split=(), kind=jnp.bfloat16):
    values = jax.random.normal(stream_key, shape, jnp.float32) * width
    if len(split) > 0:
        values = shard_levels(stream_key, shape, split, -0.22, 0.18) * values
    return jnp.clip(values, min=-reach, max=reach).astype(kind)


def setup_inputs(seed: int = 0) -> dict:
    keys = jax.random.split(jax.random.key(seed), 10)
    queries = draw_queries(jax.random.fold_in(keys[9], 71), 0)
    key_heads = draw_key_heads(jax.random.fold_in(keys[9], 71), 0)
    projected_value_heads = noise(keys[2], (SEQUENCE_TOKENS, KEY_VALUE_HEADS * HEAD_SIZE), 1.0, 5.0, ((0, 8), (1, 4)))
    sink_logit_table = jnp.clip(4.0 * jax.random.uniform(keys[3], (QUERY_HEADS,), jnp.float32) ** shard_levels(keys[3], (QUERY_HEADS,), ((0, 4),), -0.2, 0.2), 0.0, 4.0)
    out_weight = noise(keys[4], (QUERY_HEADS * HEAD_SIZE, D), 0.25, 1.5, ((0, 4),))
    residual = draw_residual(jax.random.fold_in(keys[9], 71), 0)
    norm_gain = jnp.clip(1.0 + 0.18 * jax.random.normal(keys[6], (D,), jnp.float32), 0.099609375, 1.8984375).astype(jnp.bfloat16)
    up_weight = noise(keys[7], (D, FF), D ** -0.5, 0.109375, ((0, 8), (1, 4)))
    down_weight = noise(keys[8], (FF, D), FF ** -0.5, 0.0546875, ((0, 4), (1, 8)))
    return dict(queries=queries, key_heads=key_heads, projected_value_heads=projected_value_heads, sink_logit_table=sink_logit_table, out_weight=out_weight, residual=residual, norm_gain=norm_gain, up_weight=up_weight, down_weight=down_weight)


epsilon = 1e-06

def attend(queries, key_heads, projected_value_heads, sink_logit_table):
    sequence_length = queries.shape[0]
    block_count = sequence_length // WINDOW_SPAN
    group_count = QUERY_HEADS // KEY_VALUE_HEADS
    query_block_list = queries.astype(jnp.float32).reshape(block_count, WINDOW_SPAN, KEY_VALUE_HEADS, group_count, HEAD_SIZE)

    def banded(source_rows):
        padded_rows = jnp.pad(source_rows.astype(jnp.float32).reshape(sequence_length, KEY_VALUE_HEADS, HEAD_SIZE), ((WINDOW_SPAN, 0), (0, 0), (0, 0)))
        padded_rows = padded_rows.reshape(block_count + 1, WINDOW_SPAN, KEY_VALUE_HEADS, HEAD_SIZE)
        return jnp.concatenate([padded_rows[:-1], padded_rows[1:]], axis=1)
    key_band = banded(key_heads)
    value_band = banded(projected_value_heads)
    scores = jnp.einsum('nqkgd,nskd->nkgqs', query_block_list, key_band) * HEAD_SIZE ** (-0.5)
    within = jnp.arange(WINDOW_SPAN)[:, None]
    column = jnp.arange(2 * WINDOW_SPAN)[None, :]
    distance = WINDOW_SPAN + within - column
    valid = (distance >= 0) & (distance < WINDOW_SPAN)
    key_pos = jnp.arange(block_count)[:, None] * WINDOW_SPAN + jnp.arange(2 * WINDOW_SPAN)[None, :] - WINDOW_SPAN
    allowed = valid[None] & (key_pos >= 0)[:, None, :]
    allowed = allowed[:, None, None]
    head_sink_logit = sink_logit_table.astype(jnp.float32).reshape(KEY_VALUE_HEADS, group_count)[None, :, :, None, None]
    masked = jnp.where(allowed, scores, -1e+30)
    ceiling = jnp.maximum(lax.optimization_barrier(jnp.max(masked, axis=-1, keepdims=True)), head_sink_logit)
    powers = jnp.where(allowed, jnp.exp(masked - ceiling), 0.0)
    denom = lax.optimization_barrier(jnp.sum(powers, axis=-1, keepdims=True)) + jnp.exp(head_sink_logit - ceiling)
    probs = (powers / denom).astype(jnp.bfloat16)
    output = jnp.einsum('nkgqs,nskd->nqkgd', probs.astype(jnp.float32), value_band)
    return output.reshape(sequence_length, QUERY_HEADS * HEAD_SIZE).astype(jnp.bfloat16)

def reference(queries, key_heads, projected_value_heads, sink_logit_table, out_weight, residual, norm_gain, up_weight, down_weight):
    attended = attend(queries, key_heads, projected_value_heads, sink_logit_table)
    head_cols = QUERY_HEADS * HEAD_SIZE // N_TP
    mixed = jnp.zeros(residual.shape, jnp.float32)
    for group in range(N_TP):
        part = jnp.dot(attended[:, group * head_cols:(group + 1) * head_cols], out_weight[group * head_cols:(group + 1) * head_cols], preferred_element_type=jnp.float32)
        part = lax.optimization_barrier(part.astype(jnp.bfloat16))
        mixed = mixed + part.astype(jnp.float32)
    stream = lax.optimization_barrier((residual.astype(jnp.float32) + mixed).astype(jnp.bfloat16)).astype(jnp.float32)
    mean_square = lax.optimization_barrier(jnp.mean(stream * stream, axis=-1, keepdims=True)) + epsilon
    normed = (stream * lax.rsqrt(mean_square) * norm_gain.astype(jnp.float32)).astype(jnp.bfloat16)
    unit_cols = FF // N_TP
    branch_sum = jnp.zeros(residual.shape, jnp.float32)
    for group in range(N_TP):
        hidden_pre = jnp.dot(normed, up_weight[:, group * unit_cols:(group + 1) * unit_cols], preferred_element_type=jnp.float32)
        activated = jnp.square(jax.nn.relu(hidden_pre)).astype(jnp.bfloat16)
        branch = jnp.dot(activated, down_weight[group * unit_cols:(group + 1) * unit_cols], preferred_element_type=jnp.float32)
        branch = lax.optimization_barrier(branch.astype(jnp.bfloat16))
        branch_sum = branch_sum + branch.astype(jnp.float32)
    return (stream + branch_sum).astype(jnp.bfloat16)
```

```python
import jax
import jax.numpy as jnp
from jax import lax
from jax.sharding import Mesh, PartitionSpec as P

D = 3072
HEAD_SIZE = 64
WINDOW_SPAN = 128


epsilon = 1e-06


def attend(queries, key_heads, projected_value_heads, sink_logit_table, previous, offset):
    row_count = queries.shape[0]
    kv_cols = key_heads.shape[1]
    kv_local = kv_cols // HEAD_SIZE
    group_count = queries.shape[1] // kv_cols
    block_count = row_count // WINDOW_SPAN
    extended_keys = jnp.concatenate([previous[:, :kv_cols], key_heads], axis=0)
    extended_values = jnp.concatenate([previous[:, kv_cols:], projected_value_heads], axis=0)

    def banded(source_rows):
        shaped = source_rows.reshape(block_count + 1, WINDOW_SPAN, kv_local, HEAD_SIZE)
        return jnp.concatenate([shaped[:-1], shaped[1:]], axis=1)

    key_band = banded(extended_keys)
    value_band = banded(extended_values)
    query_block_list = queries.reshape(block_count, WINDOW_SPAN, kv_local, group_count, HEAD_SIZE)
    scores = jnp.einsum(
        "nqkgd,nskd->nkgqs", query_block_list, key_band, preferred_element_type=jnp.float32
    ) * HEAD_SIZE ** (-0.5)
    within = jnp.arange(WINDOW_SPAN)[:, None]
    column = jnp.arange(2 * WINDOW_SPAN)[None, :]
    distance = WINDOW_SPAN + within - column
    valid = (distance >= 0) & (distance < WINDOW_SPAN)
    key_pos = (
        offset
        + jnp.arange(block_count)[:, None] * WINDOW_SPAN
        + jnp.arange(2 * WINDOW_SPAN)[None, :]
        - WINDOW_SPAN
    )
    allowed = valid[None] & (key_pos >= 0)[:, None, :]
    allowed = allowed[:, None, None]
    head_sink_logit = sink_logit_table.reshape(kv_local, group_count)[None, :, :, None, None]
    masked = jnp.where(allowed, scores, -1e30)
    ceiling = jnp.maximum(jnp.max(masked, axis=-1, keepdims=True), head_sink_logit)
    powers = jnp.where(allowed, jnp.exp(masked - ceiling), 0.0)
    denom = jnp.sum(powers, axis=-1, keepdims=True) + jnp.exp(head_sink_logit - ceiling)
    probs = (powers / denom).astype(jnp.bfloat16)
    output = jnp.einsum("nkgqs,nskd->nqkgd", probs, value_band, preferred_element_type=jnp.float32)
    return output.astype(jnp.bfloat16).reshape(row_count, queries.shape[1])


SP = ("zh", "zl", "x")
TP = ("y", "c")
SWAP = [(0, 1), (1, 0)]
CHUNKS = 2


def shift(block, axis, k):
    n = lax.axis_size(axis)
    return lax.ppermute(block, axis, [(i, (i + k) % n) for i in range(n)])


def spread(pieces, axis):
    n = lax.axis_size(axis)
    me = lax.axis_index(axis)
    out = []
    for block, at in pieces:
        for k in range(1, n):
            out.append((shift(block, axis, k), {**at, axis: (me - k + n) % n}))
    return out


def gather_weight(weight, col_major):
    zl, zh, x = (lax.axis_index(a) for a in ("zl", "zh", "x"))
    dim = 0 if col_major else 1
    half = weight.shape[dim] // 2
    mine = lax.dynamic_slice_in_dim(weight, zl * half, half, dim)
    theirs = lax.dynamic_slice_in_dim(weight, (1 - zl) * half, half, dim)
    first = [(mine, dict(zh=zh, zl=zl, x=x))]
    first.append((lax.ppermute(theirs, "zl", SWAP), dict(zh=zh, zl=1 - zl, x=x)))
    far = spread(first, "zh")
    pieces = first + far
    pieces = pieces + spread(first, "x") + spread(far, "x")
    span = weight.shape[1 - dim]
    sp_size = lax.axis_size(SP)
    shape = [0, 0]
    shape[dim] = half
    shape[1 - dim] = span * sp_size
    whole = jnp.zeros(shape, weight.dtype)
    nx, nl = lax.axis_size("x"), lax.axis_size("zl")
    for block, at in pieces:
        s = (at["zh"] * nl + at["zl"]) * nx + at["x"]
        whole = lax.dynamic_update_slice_in_dim(whole, block, s * span, 1 - dim)
    return whole


def tp_blocks(width):
    y, c = lax.axis_index("y"), lax.axis_index("c")
    ny = lax.axis_size("y")

    def start(k, other):
        return (((y + k) % ny) * 2 + (1 - c if other else c)) * width

    return start


def scatter_product(left, right, width):
    ny = lax.axis_size("y")
    start = tp_blocks(width)

    def product(k, other):
        w = lax.dynamic_slice_in_dim(right, start(k, other), width, 1)
        return jnp.dot(left, w, preferred_element_type=jnp.float32)

    total = None
    for k in list(range(1, ny)) + [0]:
        sent = product(k, True).astype(jnp.bfloat16)
        got = lax.ppermute(sent, "c", SWAP).astype(jnp.float32)
        both = product(k, False) + got
        if k:
            both = shift(both.astype(jnp.bfloat16), "y", k).astype(jnp.float32)
        total = both if total is None else total + both
    return total


def gather_tokens(own):
    rows, width = own.shape
    y, c = lax.axis_index("y"), lax.axis_index("c")
    pieces = [(own, dict(r=0, y=y)), (lax.ppermute(own, "zl", SWAP), dict(r=1, y=y))]
    pieces = pieces + spread(pieces, "y")
    pieces = [(b, {**at, "c": c}) for b, at in pieces]
    pieces = pieces + spread(pieces, "c")
    whole = jnp.zeros((2 * rows, width * lax.axis_size(TP)), own.dtype)
    for block, at in pieces:
        whole = lax.dynamic_update_slice(
            whole, block, (at["r"] * rows, (at["y"] * 2 + at["c"]) * width)
        )
    return whole


def body(
    queries,
    key_heads,
    projected_value_heads,
    sink_logit_table,
    out_weight,
    residual,
    norm_gain,
    up_weight,
    down_weight,
):
    row_count = queries.shape[0]
    offset = lax.axis_index(SP) * row_count
    width = residual.shape[1]
    tail = jnp.concatenate(
        [key_heads[row_count - WINDOW_SPAN :], projected_value_heads[row_count - WINDOW_SPAN :]],
        axis=1,
    )
    sp_size = lax.axis_size(SP)
    previous = lax.ppermute(tail, SP, [(i, i + 1) for i in range(sp_size - 1)])
    up_whole = gather_weight(up_weight, False)
    down_whole = gather_weight(down_weight, True)
    attended = attend(queries, key_heads, projected_value_heads, sink_logit_table, previous, offset)
    gain = norm_gain.astype(jnp.float32)
    rows = row_count // CHUNKS
    streams, scales, tokens = [], [], []
    for i in range(CHUNKS):
        part = slice(i * rows, (i + 1) * rows)
        mixed = scatter_product(attended[part], out_weight, width)
        stream = (residual[part].astype(jnp.float32) + mixed).astype(jnp.bfloat16)
        stream = lax.optimization_barrier(stream)
        wide = stream.astype(jnp.float32)
        gained = (wide * gain).astype(jnp.bfloat16)
        tokens.append(gather_tokens(gained))
        squares = lax.psum(jnp.sum(wide * wide, axis=1, keepdims=True), TP)
        scale = lax.rsqrt(squares / D + epsilon)
        scales.append(jnp.concatenate([scale, lax.ppermute(scale, "zl", SWAP)], axis=0))
        streams.append(wide)
    results = []
    for i in range(CHUNKS):
        hidden = jnp.dot(tokens[i], up_whole, preferred_element_type=jnp.float32) * scales[i]
        activated = jnp.square(jax.nn.relu(hidden)).astype(jnp.bfloat16)
        theirs = scatter_product(activated[rows:], down_whole, width)
        got = lax.ppermute(theirs.astype(jnp.bfloat16), "zl", SWAP).astype(jnp.float32)
        branch = scatter_product(activated[:rows], down_whole, width) + got
        results.append((streams[i] + branch).astype(jnp.bfloat16))
    return jnp.concatenate(results, axis=0)


def solution(mesh):
    sp, tp = mesh.shape["sp"], mesh.shape["tp"]
    inner = Mesh(mesh.devices.reshape(sp // 4, 2, 2, tp // 2, 2), SP + TP)
    return jax.shard_map(
        body,
        mesh=inner,
        in_specs=(
            P(SP, TP),
            P(SP, TP),
            P(SP, TP),
            P(TP),
            P(TP, None),
            P(SP, TP),
            P(TP),
            P(SP, TP),
            P(TP, SP),
        ),
        out_specs=P(SP, TP),
        check_vma=False,
    )
```

```python
import jax
import jax.numpy as jnp
from jax import lax
from jax.sharding import Mesh, PartitionSpec as P

D = 3072
HEAD_SIZE = 64
WINDOW_SPAN = 128


epsilon = 1e-06


def attend(queries, key_heads, projected_value_heads, sink_logit_table, previous, offset):
    row_count = queries.shape[0]
    kv_cols = key_heads.shape[1]
    kv_local = kv_cols // HEAD_SIZE
    group_count = queries.shape[1] // kv_cols
    block_count = row_count // WINDOW_SPAN
    extended_keys = jnp.concatenate([previous[:, :kv_cols], key_heads], axis=0)
    extended_values = jnp.concatenate([previous[:, kv_cols:], projected_value_heads], axis=0)

    def banded(source_rows):
        shaped = source_rows.reshape(block_count + 1, WINDOW_SPAN, kv_local, HEAD_SIZE)
        return jnp.concatenate([shaped[:-1], shaped[1:]], axis=1)

    key_band = banded(extended_keys)
    value_band = banded(extended_values)
    query_block_list = queries.reshape(block_count, WINDOW_SPAN, kv_local, group_count, HEAD_SIZE)
    scores = jnp.einsum(
        "nqkgd,nskd->nkgqs", query_block_list, key_band, preferred_element_type=jnp.float32
    ) * HEAD_SIZE ** (-0.5)
    within = jnp.arange(WINDOW_SPAN)[:, None]
    column = jnp.arange(2 * WINDOW_SPAN)[None, :]
    distance = WINDOW_SPAN + within - column
    valid = (distance >= 0) & (distance < WINDOW_SPAN)
    key_pos = (
        offset
        + jnp.arange(block_count)[:, None] * WINDOW_SPAN
        + jnp.arange(2 * WINDOW_SPAN)[None, :]
        - WINDOW_SPAN
    )
    allowed = valid[None] & (key_pos >= 0)[:, None, :]
    allowed = allowed[:, None, None]
    head_sink_logit = sink_logit_table.reshape(kv_local, group_count)[None, :, :, None, None]
    masked = jnp.where(allowed, scores, -1e30)
    ceiling = jnp.maximum(jnp.max(masked, axis=-1, keepdims=True), head_sink_logit)
    powers = jnp.where(allowed, jnp.exp(masked - ceiling), 0.0)
    denom = jnp.sum(powers, axis=-1, keepdims=True) + jnp.exp(head_sink_logit - ceiling)
    probs = (powers / denom).astype(jnp.bfloat16)
    output = jnp.einsum("nkgqs,nskd->nqkgd", probs, value_band, preferred_element_type=jnp.float32)
    return output.astype(jnp.bfloat16).reshape(row_count, queries.shape[1])


SP = ("zh", "zl", "x")
TP = ("y", "c")
SWAP = [(0, 1), (1, 0)]
CHUNKS = 2


def shift(block, axis, k):
    n = lax.axis_size(axis)
    return lax.ppermute(block, axis, [(i, (i + k) % n) for i in range(n)])


def spread(pieces, axis):
    n = lax.axis_size(axis)
    me = lax.axis_index(axis)
    out = []
    for block, at in pieces:
        for k in range(1, n):
            out.append((shift(block, axis, k), {**at, axis: (me - k + n) % n}))
    return out


def gate(block, after):
    return lax.optimization_barrier((block, after))


def blank(shape, after):
    zero, _ = gate(jnp.zeros((), after.dtype), after)
    return jnp.broadcast_to(zero, shape)


def gather_weights(weights):
    zl, zh, x = (lax.axis_index(a) for a in ("zl", "zh", "x"))
    nx, nl = lax.axis_size("x"), lax.axis_size("zl")
    sp_size = lax.axis_size(SP)
    results = []
    earlier = None
    for dim, weight in zip((1, 0), weights):
        half = weight.shape[dim] // 2
        span = weight.shape[1 - dim]
        mine = lax.dynamic_slice_in_dim(weight, zl * half, half, dim)
        theirs = lax.dynamic_slice_in_dim(weight, (1 - zl) * half, half, dim)
        own_at, near_at = dict(zh=zh, zl=zl, x=x), dict(zh=zh, zl=1 - zl, x=x)
        for_far = for_side = mine
        if earlier:
            near0, far0, far1 = earlier
            theirs, near0 = gate(theirs, near0)
            for_side, near0 = gate(mine, near0)
            for_far, far0 = gate(mine, far0)
        near = lax.ppermute(theirs, "zl", SWAP)
        far_own = spread([(for_far, own_at)], "zh")
        side_own = spread([(for_side, own_at)], "x")
        near_out = near
        if earlier:
            near_out, far1 = gate(near, far1)
        far_near = spread([(near_out, near_at)], "zh")
        side_near = spread([(near, near_at)], "x")
        pieces = [(mine, own_at), (near, near_at)] + far_own + far_near + side_own + side_near
        pieces += spread(far_own, "x") + spread(far_near, "x")
        earlier = (near, far_own[0][0], far_near[0][0])
        shape = [half, half]
        shape[1 - dim] = span * sp_size
        whole = blank(shape, near)
        for block, at in pieces:
            at_block = (at["zh"] * nl + at["zl"]) * nx + at["x"]
            whole = lax.dynamic_update_slice_in_dim(whole, block, at_block * span, 1 - dim)
        results.append(whole)
    return results


def tp_blocks(width):
    y, c = lax.axis_index("y"), lax.axis_index("c")
    ny = lax.axis_size("y")

    def start(k, other):
        return (((y + k) % ny) * 2 + (1 - c if other else c)) * width

    return start


def scatter_product(left, right, width):
    ny = lax.axis_size("y")
    start = tp_blocks(width)

    def product(k, other):
        w = lax.dynamic_slice_in_dim(right, start(k, other), width, 1)
        return jnp.dot(left, w, preferred_element_type=jnp.float32)

    total = None
    for k in list(range(1, ny)) + [0]:
        sent = product(k, True).astype(jnp.bfloat16)
        got = lax.ppermute(sent, "c", SWAP).astype(jnp.float32)
        both = product(k, False) + got
        if k:
            both = shift(both.astype(jnp.bfloat16), "y", k).astype(jnp.float32)
        total = both if total is None else total + both
    return total


def finish(activated, down, width, far_first):
    ny = lax.axis_size("y")
    rows = activated.shape[0] // 2
    start = tp_blocks(width)

    def product(k, other):
        w = lax.dynamic_slice_in_dim(down, start(k, other), width, 1)
        return jnp.dot(activated, w, preferred_element_type=jnp.float32)

    def moved(block, axis, k):
        return shift(block.astype(jnp.bfloat16), axis, k).astype(jnp.float32)

    mine = theirs = None
    for k in list(range(1, ny)) + [0]:
        both = product(k, False) + lax.ppermute(
            product(k, True).astype(jnp.bfloat16), "c", SWAP
        ).astype(jnp.float32)
        here, there = both[:rows], both[rows:]
        if far_first:
            here = here + moved(there, "zl", 1)
            here = moved(here, "y", k) if k else here
        else:
            if k:
                there, here = moved(there, "y", k), moved(here, "y", k)
            theirs = there if theirs is None else theirs + there
        mine = here if mine is None else mine + here
    return mine if far_first else mine + moved(theirs, "zl", 1)


def gather_tokens(own):
    rows, width = own.shape
    y, c = lax.axis_index("y"), lax.axis_index("c")
    pieces = [(own, dict(r=0, y=y)), (lax.ppermute(own, "zl", SWAP), dict(r=1, y=y))]
    pieces = pieces + spread(pieces, "y")
    pieces = [(b, {**at, "c": c}) for b, at in pieces]
    pieces = pieces + spread(pieces, "c")
    whole = blank((2 * rows, width * lax.axis_size(TP)), own)
    for block, at in pieces:
        whole = lax.dynamic_update_slice(
            whole, block, (at["r"] * rows, (at["y"] * 2 + at["c"]) * width)
        )
    return whole


def body(
    queries,
    key_heads,
    projected_value_heads,
    sink_logit_table,
    out_weight,
    residual,
    norm_gain,
    up_weight,
    down_weight,
):
    row_count = queries.shape[0]
    offset = lax.axis_index(SP) * row_count
    width = residual.shape[1]
    tail = jnp.concatenate(
        [key_heads[row_count - WINDOW_SPAN :], projected_value_heads[row_count - WINDOW_SPAN :]],
        axis=1,
    )
    sp_size = lax.axis_size(SP)
    previous = lax.ppermute(tail, SP, [(i, i + 1) for i in range(sp_size - 1)])
    gain_pieces = [(norm_gain[None], dict(y=lax.axis_index("y")))]
    gain_pieces += spread(gain_pieces, "y")
    gain_pieces = [(g, {**at, "c": lax.axis_index("c")}) for g, at in gain_pieces]
    gain_pieces += spread(gain_pieces, "c")
    gain = jnp.zeros((1, width * lax.axis_size(TP)), norm_gain.dtype)
    for block, at in gain_pieces:
        gain = lax.dynamic_update_slice(gain, block, (0, (at["y"] * 2 + at["c"]) * width))
    up_weight, down_weight, previous, gain = lax.optimization_barrier(
        (up_weight, down_weight, previous, gain)
    )
    gain = gain.astype(jnp.float32)
    up_whole, down_whole = gather_weights((up_weight, down_weight))
    attended = attend(queries, key_heads, projected_value_heads, sink_logit_table, previous, offset)
    rows = row_count // CHUNKS
    streams, tokens = [], []
    for i in range(CHUNKS):
        part = slice(i * rows, (i + 1) * rows)
        mixed = scatter_product(attended[part], out_weight, width)
        stream = (residual[part].astype(jnp.float32) + mixed).astype(jnp.bfloat16)
        stream = lax.optimization_barrier(stream)
        tokens.append(gather_tokens(stream))
        streams.append(stream.astype(jnp.float32))
    results = []
    for i in range(CHUNKS):
        wide = tokens[i].astype(jnp.float32)
        scale = lax.rsqrt(jnp.sum(wide * wide, axis=1, keepdims=True) / D + epsilon)
        gained = (wide * gain).astype(jnp.bfloat16)
        hidden = jnp.dot(gained, up_whole, preferred_element_type=jnp.float32) * scale
        activated = jnp.square(jax.nn.relu(hidden)).astype(jnp.bfloat16)
        branch = finish(activated, down_whole, width, i % 2 == 1)
        results.append((streams[i] + branch).astype(jnp.bfloat16))
    return jnp.concatenate(results, axis=0)


def solution(mesh):
    sp, tp = mesh.shape["sp"], mesh.shape["tp"]
    inner = Mesh(mesh.devices.reshape(sp // 4, 2, 2, tp // 2, 2), SP + TP)
    return jax.shard_map(
        body,
        mesh=inner,
        in_specs=(
            P(SP, TP),
            P(SP, TP),
            P(SP, TP),
            P(TP),
            P(TP, None),
            P(SP, TP),
            P(TP),
            P(SP, TP),
            P(TP, SP),
        ),
        out_specs=P(SP, TP),
        check_vma=False,
    )
```
